256 devices in a mesh: fs: 64 (over z, x, core), tp: 4 (over y).
Axes of the slice: x: 4, y: 4, z: 8, core: 2. Of those that a mesh axis runs over, the one named last changes fastest.
Arguments:
- late_input: bfloat16 [32768, 2048], P(('fs', 'tp')), may hold values from -6 to 6
- norm_gain: bfloat16 [2048], replicated, may hold values from 0.099609375 to 1.8984375
- gate_weight: bfloat16 [2048, 2816], P('fs', 'tp'), may hold values from -0.125 to 0.125
- up_weight: bfloat16 [2048, 2816], P('fs', 'tp'), may hold values from -0.125 to 0.125
- down_weight: bfloat16 [2048, 2816], P('fs', 'tp'), may hold values from -0.109375 to 0.109375
- early_input: bfloat16 [32768, 2048], P(('fs', 'tp')), may hold values from -6 to 6
- cotangent: bfloat16 [32768, 2048], P(('fs', 'tp')), may hold values from -24 to 24
- gate_sum: float32 [2048, 2816], P('fs', 'tp'), may hold values from -192 to 192
- up_sum: float32 [2048, 2816], P('fs', 'tp'), may hold values from -192 to 192
- down_sum: float32 [2048, 2816], P('fs', 'tp'), may hold values from -192 to 192
- gain_sum: float32 [2048], replicated, may hold values from -192 to 192
Outputs:
- late_out: bfloat16 [32768, 2048], P(('fs', 'tp'))
- early_grad: bfloat16 [32768, 2048], P(('fs', 'tp'))
- gate_sum_out: float32 [2048, 2816], P('fs', 'tp')
- up_sum_out: float32 [2048, 2816], P('fs', 'tp')
- down_sum_out: float32 [2048, 2816], P('fs', 'tp')
- gain_sum_out: float32 [2048], replicated
The draws below stay inside these ranges and needn't reach their ends.
All inputs are finite; a program needn't handle non-finite values.
Results may differ from the reference program's by a relative error of at most 0.008.
Values may be sent and summed in bfloat16 or wider, within the bound.
No kernel may reach another device: no remote copies, remote signals or barrier semaphores. Data moves between devices by JAX's collectives and lax.ppermute only.
A program may use at most 128 MiB of HBM per device.

```python
import jax
import jax.numpy as jnp
from jax import lax

D = 2048
FF = 2816
TOKENS = 32768
N_TP = 4


def with_spikes(drawn, stream_key, source, target, blocks, factor):
    owner, partner = [(jnp.arange(drawn.shape[axis_at]) // (drawn.shape[axis_at] // blocks)).reshape([-1 if axis == axis_at else 1 for axis in range(drawn.ndim)]) for axis_at in (source, target)]
    chosen = jax.random.permutation(stream_key, blocks)[partner]
    strong = (owner == chosen) | (owner == (partner + blocks // 2) % blocks)
    return jnp.where(strong, factor * drawn, drawn)


def block_levels(rng, extent, pieces, least, high):
    level = 1.0
    for axis_at, shards_of in pieces:
        draws = jax.random.uniform(jax.random.fold_in(jax.random.fold_in(rng, 6), axis_at), (shards_of,), jnp.float32, least / len(pieces), high / len(pieces))
        level = level * jnp.repeat(jnp.exp(draws), extent[axis_at] // shards_of).reshape((-1,) + (1,) * (len(extent) - 1 - axis_at))
    return level


def scatter_about(stream_key, shape, deviation, most, split=(), dtype=jnp.bfloat16):
    level = block_levels(stream_key, shape, split, -0.22, 0.18) if split else 1.0
    result = jax.random.normal(stream_key, shape, jnp.float32) * deviation * level
    return jnp.minimum(jnp.maximum(result, -most), most).astype(dtype)


def bell_draw_with(key, extent, deviation, limit, shards, heavy, dtype=jnp.bfloat16):
    entries = deviation * jax.random.normal(key, extent, jnp.float32)
    if shards:
        entries = entries * block_levels(key, extent, shards, -0.22, 0.18)
    return jnp.clip(with_spikes(entries, jax.random.fold_in(key, 3), *heavy), -limit, limit).astype(dtype)


def setup_inputs(seed: int = 0) -> dict:
    keys = jax.random.split(jax.random.key(seed), 12)
    return {
        "late_input": scatter_about(keys[0], (TOKENS, D), 1.0, 6.0, ((0, 256),)),
        "norm_gain": jnp.clip(1.0 + 0.18 * jax.random.normal(keys[1], (D,), jnp.float32), 0.099609375, 1.8984375).astype(jnp.bfloat16),
        "gate_weight": scatter_about(keys[2], (D, FF), D ** -0.5, 0.125, ((0, 64), (1, 4))),
        "up_weight": scatter_about(keys[3], (D, FF), D ** -0.5, 0.125, ((0, 64), (1, 4))),
        "down_weight": scatter_about(keys[4], (D, FF), FF ** -0.5, 0.109375, ((0, 64), (1, 4))),
        "early_input": scatter_about(keys[5], (TOKENS, D), 1.0, 6.0, ((0, 256),)),
        "cotangent": bell_draw_with(keys[6], (TOKENS, D), 1.0, 24.0, ((0, 256),), (0, 1, 256, 6.0)),
        "gate_sum": scatter_about(keys[7], (D, FF), 32.0, 192.0, ((0, 64), (1, 4)), jnp.float32),
        "up_sum": scatter_about(keys[8], (D, FF), 32.0, 192.0, ((0, 64), (1, 4)), jnp.float32),
        "down_sum": scatter_about(keys[9], (D, FF), 32.0, 192.0, ((0, 64), (1, 4)), jnp.float32),
        "gain_sum": scatter_about(keys[10], (D,), 32.0, 192.0, (), jnp.float32),
    }


epsilon = 1e-05

def normalize(source, gain_f):
    values = source.astype(jnp.float32)
    scale = lax.rsqrt(lax.optimization_barrier(jnp.mean(values * values, axis=-1, keepdims=True)) + epsilon)
    return ((values * scale * gain_f).astype(jnp.bfloat16), scale, values)

def blocked(pairs):
    width = FF // N_TP
    total = None
    for block in range(N_TP):
        partial_value = None
        for left, right in pairs:
            term = jnp.dot(left[:, block * width:(block + 1) * width], right[:, block * width:(block + 1) * width].T, preferred_element_type=jnp.float32)
            partial_value = term if partial_value is None else partial_value + term
        rounded = lax.optimization_barrier(partial_value.astype(jnp.bfloat16)).astype(jnp.float32)
        total = rounded if total is None else total + rounded
    return total

def reference(late_input, norm_gain, gate_weight, up_weight, down_weight, early_input, cotangent, gate_sum, up_sum, down_sum, gain_sum):
    gain_f = norm_gain.astype(jnp.float32)
    normed, scale, values = normalize(late_input, gain_f)
    gate = jnp.dot(normed, gate_weight, preferred_element_type=jnp.float32)
    upper = jnp.dot(normed, up_weight, preferred_element_type=jnp.float32)
    hidden = (jax.nn.silu(gate) * upper).astype(jnp.bfloat16)
    mixed = blocked([(hidden, down_weight)])
    late_out = (values + 0.5 * mixed).astype(jnp.bfloat16)
    normed_e, scale_e, values_e = normalize(early_input, gain_f)
    gate_e = jnp.dot(normed_e, gate_weight, preferred_element_type=jnp.float32)
    upper_e = jnp.dot(normed_e, up_weight, preferred_element_type=jnp.float32)
    sigma_e = jax.nn.sigmoid(gate_e)
    hidden_e = (gate_e * sigma_e * upper_e).astype(jnp.bfloat16)
    d_hidden = 0.5 * jnp.dot(cotangent, down_weight, preferred_element_type=jnp.float32)
    d_gate = (d_hidden * upper_e * sigma_e * (1.0 + gate_e * (1.0 - sigma_e))).astype(jnp.bfloat16)
    d_up = (d_hidden * gate_e * sigma_e).astype(jnp.bfloat16)
    d_normed = blocked([(d_gate, gate_weight), (d_up, up_weight)])
    scaled_grad = d_normed * gain_f
    early_grad = (cotangent.astype(jnp.float32) + scale_e * scaled_grad - values_e * scale_e ** 3 * lax.optimization_barrier(jnp.mean(values_e * scaled_grad, axis=-1, keepdims=True))).astype(jnp.bfloat16)
    gain_sum_out = gain_sum + lax.optimization_barrier(jnp.sum(d_normed * values_e * scale_e, axis=0))
    gate_sum_out = gate_sum + jnp.dot(normed_e.T, d_gate, preferred_element_type=jnp.float32)
    up_sum_out = up_sum + jnp.dot(normed_e.T, d_up, preferred_element_type=jnp.float32)
    down_sum_out = down_sum + 0.5 * jnp.dot(cotangent.T, hidden_e, preferred_element_type=jnp.float32)
    return (late_out, early_grad, gate_sum_out, up_sum_out, down_sum_out, gain_sum_out)
```

```python
import jax
import jax.numpy as jnp
from jax import lax
from jax.experimental import pallas as pl
from jax.experimental.pallas import tpu as pltpu
from jax.sharding import Mesh
from jax.sharding import PartitionSpec as P

Z, X, C, Y = "fs_0", "fs_1", "fs_2", "tp"
FS = (Z, X, C)
FS_TP = (Z, X, C, Y)


epsilon = 1e-05
bf16, f32 = jnp.bfloat16, jnp.float32


def shift(value, axis, k):
    n = lax.axis_size(axis)
    return lax.ppermute(value, axis, [(i, (i + k) % n) for i in range(n)])


def partner(value, axis, bit):
    n = lax.axis_size(axis)
    return lax.ppermute(value, axis, [(i, i ^ bit) for i in range(n)])


def at(value, index, axis):
    return lax.dynamic_index_in_dim(value, index, axis, keepdims=False)


def normalize(source, gain_f):
    values = source.astype(f32)
    scale = lax.rsqrt(jnp.mean(values * values, axis=-1, keepdims=True) + epsilon)
    return ((values * scale * gain_f).astype(bf16), scale, values)


def dot(left, right, over):
    return lax.dot_general(left, right, ((over[0], over[1]), ((), ())), preferred_element_type=f32)


def tokens_everywhere(value):
    half = value.shape[0] // 2
    behind, ahead = shift(value, Y, 1), shift(value, Y, -1)
    near = jnp.concatenate([value, behind, ahead], axis=0)
    far = jnp.concatenate([shift(behind[:half], Y, 1), shift(ahead[half:], Y, -1)], axis=0)
    return jnp.concatenate([near, far, shift(near, C, 1), shift(far, C, 1)], axis=0)


def tokens_summed(own, recv):
    mine = own + recv.astype(f32)
    q = mine.shape[1] // 4
    half = q // 2
    far = mine[:, 3 * q :].astype(bf16)
    u = shift(far[:, :half], Y, 1)
    v = shift(far[:, half:], Y, -1)
    ahead, behind = mine[:, 2 * q : 3 * q], mine[:, q : 2 * q]
    up = jnp.concatenate([ahead[:, :half] + u.astype(f32), ahead[:, half:]], axis=1)
    down = jnp.concatenate([behind[:, :half], behind[:, half:] + v.astype(f32)], axis=1)
    r = shift(up.astype(bf16), Y, 1)
    s = shift(down.astype(bf16), Y, -1)
    return mine[:, :q] + r.astype(f32) + s.astype(f32)


def weights_everywhere(mine, theirs):
    z, x, c = lax.axis_index(Z), lax.axis_index(X), lax.axis_index(C)
    nz, nx = lax.axis_size(Z), lax.axis_size(X)
    rows, cols = mine.shape
    other = shift(theirs, C, 1)
    piece = jnp.where(
        c == 0,
        jnp.concatenate([mine, other], axis=0),
        jnp.concatenate([other, mine], axis=0),
    )
    plane = jnp.zeros((nx, 2 * rows, cols), mine.dtype)
    for k in range(nx):
        arrived = piece if k == 0 else shift(piece, X, k)
        plane = lax.dynamic_update_slice(plane, arrived[None], ((x - k) % nx, 0, 0))
    plane = plane.reshape(-1, cols).T

    whole = jnp.zeros((nz, *plane.shape), mine.dtype)

    def put(whole, arrived, k, at_column=0):
        return lax.dynamic_update_slice(whole, arrived[None], ((z + k) % nz, at_column, 0))

    whole = put(whole, plane, 0)
    fore, back = plane, plane
    for k in range(1, nz // 2):
        fore, back = shift(fore, Z, 1), shift(back, Z, -1)
        whole = put(whole, fore, -k)
        whole = put(whole, back, k)
    half = cols // 2
    whole = put(whole, shift(fore[:half], Z, 1), nz // 2, 0)
    whole = put(whole, shift(back[half:], Z, -1), nz // 2, half)
    return whole


def rows_summed(grads):
    z, x, c = lax.axis_index(Z), lax.axis_index(X), lax.axis_index(C)
    nz, nx = lax.axis_size(Z), lax.axis_size(X)
    cols = grads.shape[1]

    def part(k):
        return at(grads, (z + k) % nz, 0).astype(f32)

    half = cols // 2
    far = part(nz // 2).astype(bf16)
    fore = shift(far[:half], Z, 1)
    back = shift(far[half:], Z, -1)
    for k in range(nz // 2 - 1, 0, -1):
        a, b = part(k), part(-k)
        if k == nz // 2 - 1:
            a = jnp.concatenate([a[:half] + fore.astype(f32), a[half:]], axis=0)
            b = jnp.concatenate([b[:half], b[half:] + back.astype(f32)], axis=0)
        else:
            a, b = a + fore.astype(f32), b + back.astype(f32)
        fore, back = shift(a.astype(bf16), Z, 1), shift(b.astype(bf16), Z, -1)
    plane = part(0) + fore.astype(f32) + back.astype(f32)
    plane = plane.T.reshape(nx, -1, cols)
    mine = at(plane, x, 0)
    for k in range(1, nx):
        mine = mine + shift(at(plane, (x + k) % nx, 0).astype(bf16), X, k).astype(f32)
    mine = mine.reshape(2, -1, cols)
    return at(mine, c, 0), shift(at(mine, 1 - c, 0).astype(bf16), C, 1).astype(f32)


def hidden_kernel(width, w_ref, tok_ref, d_ref, dt_ref, h_ref):
    nz, _, depth = w_ref.shape
    features = nz * depth

    def product(first, last, column):
        total = None
        for k in range(nz):
            left = w_ref[k, first:last]
            right = tok_ref[:, column + k * depth : column + (k + 1) * depth]
            term = dot(left, right, ((1,), (1,)))
            total = term if total is None else total + term
        return total

    both = product(0, 2 * width, 0)
    gate, upper = both[:width], both[width:]
    d_hidden = 0.5 * product(2 * width, 3 * width, features)
    sigma = jax.nn.sigmoid(gate)
    hidden = gate * sigma * upper
    d_gate = d_hidden * upper * sigma * (1.0 + gate * (1.0 - sigma))
    d_up = d_hidden * gate * sigma
    d_ref[:width] = d_gate.astype(bf16)
    d_ref[width : 2 * width] = d_up.astype(bf16)
    d_ref[2 * width :] = hidden.astype(bf16)
    dt_ref[...] = jnp.concatenate([d_gate, d_up], axis=0).T.astype(bf16)
    late = product(0, 2 * width, 2 * features)
    h_ref[...] = (jax.nn.silu(late[:width]) * late[width:]).T.astype(bf16)


def hidden_units(whole, tokens):
    nz, cols, depth = whole.shape
    width = cols // 3
    count, wide = tokens.shape
    block = 256
    return pl.pallas_call(
        lambda *refs: hidden_kernel(width, *refs),
        grid=(count // block,),
        in_specs=[
            pl.BlockSpec((nz, cols, depth), lambda i: (0, 0, 0)),
            pl.BlockSpec((block, wide), lambda i: (i, 0)),
        ],
        out_specs=[
            pl.BlockSpec((cols, block), lambda i: (0, i)),
            pl.BlockSpec((block, 2 * width), lambda i: (i, 0)),
            pl.BlockSpec((block, width), lambda i: (i, 0)),
        ],
        out_shape=[
            jax.ShapeDtypeStruct((cols, count), bf16),
            jax.ShapeDtypeStruct((count, 2 * width), bf16),
            jax.ShapeDtypeStruct((count, width), bf16),
        ],
        compiler_params=pltpu.CompilerParams(vmem_limit_bytes=48 << 20),
        cost_estimate=pl.CostEstimate(
            flops=2 * count * features_of(whole) * 5 * width,
            bytes_accessed=2 * (whole.size + tokens.size),
            transcendentals=2 * count * width,
        ),
        name="hidden_units",
    )(whole, tokens)


def features_of(whole):
    return whole.shape[0] * whole.shape[2]


def grads_kernel(width, d_ref, normed_ref, cot_ref, out_ref):
    out_ref[0, : 2 * width] = dot(d_ref[: 2 * width], normed_ref[...], ((1,), (0,))).astype(bf16)
    out_ref[0, 2 * width :] = (0.5 * dot(d_ref[2 * width :], cot_ref[...], ((1,), (0,)))).astype(bf16)


def weight_grads(d, tokens, nz, depth):
    cols, count = d.shape
    return pl.pallas_call(
        lambda *refs: grads_kernel(cols // 3, *refs),
        grid=(nz,),
        in_specs=[
            pl.BlockSpec((cols, count), lambda i: (0, 0)),
            pl.BlockSpec((count, depth), lambda i: (0, i)),
            pl.BlockSpec((count, depth), lambda i: (0, nz + i)),
        ],
        out_specs=pl.BlockSpec((1, cols, depth), lambda i: (i, 0, 0)),
        out_shape=jax.ShapeDtypeStruct((nz, cols, depth), bf16),
        compiler_params=pltpu.CompilerParams(vmem_limit_bytes=32 << 20),
        cost_estimate=pl.CostEstimate(
            flops=2 * cols * count * nz * depth,
            bytes_accessed=2 * (cols * count + 2 * count * nz * depth + cols * nz * depth),
            transcendentals=0,
        ),
        name="weight_grads",
    )(d, tokens, tokens)


def outputs_kernel(width, d_ref, h_ref, w_ref, normed_ref, own_ref, send_ref, gain_ref):
    rows = own_ref.shape[1]
    early = dot(d_ref[...], w_ref[0, : 2 * width], ((1,), (0,)))
    gain_ref[0] = jnp.sum(early * normed_ref[...].astype(f32), axis=0, keepdims=True)
    own_ref[0] = early[:rows]
    send_ref[0] = early[rows:].astype(bf16)
    late = dot(h_ref[...], w_ref[0, 2 * width :], ((1,), (0,)))
    own_ref[1] = late[:rows]
    send_ref[1] = late[rows:].astype(bf16)


def partial_outputs(d, h, whole, tokens):
    nz, cols, depth = whole.shape
    width = cols // 3
    count = d.shape[0]
    features = nz * depth
    return pl.pallas_call(
        lambda *refs: outputs_kernel(width, *refs),
        grid=(nz,),
        in_specs=[
            pl.BlockSpec((count, 2 * width), lambda i: (0, 0)),
            pl.BlockSpec((count, width), lambda i: (0, 0)),
            pl.BlockSpec((1, cols, depth), lambda i: (i, 0, 0)),
            pl.BlockSpec((count, depth), lambda i: (0, i)),
        ],
        out_specs=[
            pl.BlockSpec((2, count // 2, depth), lambda i: (0, 0, i)),
            pl.BlockSpec((2, count // 2, depth), lambda i: (0, 0, i)),
            pl.BlockSpec((1, 1, depth), lambda i: (i, 0, 0)),
        ],
        out_shape=[
            jax.ShapeDtypeStruct((2, count // 2, features), f32),
            jax.ShapeDtypeStruct((2, count // 2, features), bf16),
            jax.ShapeDtypeStruct((nz, 1, depth), f32),
        ],
        compiler_params=pltpu.CompilerParams(vmem_limit_bytes=32 << 20),
        cost_estimate=pl.CostEstimate(
            flops=2 * count * features * cols,
            bytes_accessed=14 * count * features,
            transcendentals=0,
        ),
        name="partial_outputs",
    )(d, h, whole, tokens)


def summed_everywhere(value):
    for axis in (C, Y, X, Z):
        bit = 1
        while bit < lax.axis_size(axis):
            value = value + partner(value, axis, bit)
            bit *= 2
    return value


def per_device(
    late_input,
    norm_gain,
    gate_weight,
    up_weight,
    down_weight,
    early_input,
    cotangent,
    gate_sum,
    up_sum,
    down_sum,
    gain_sum,
):
    first = lax.axis_index(C) == 0
    width = gate_weight.shape[1] // 2
    low, high = [
        jnp.concatenate(
            [w[:, h * width : (h + 1) * width] for w in (gate_weight, up_weight, down_weight)],
            axis=1,
        )
        for h in range(2)
    ]
    mine, theirs = jnp.where(first, low, high), jnp.where(first, high, low)
    gain_f = norm_gain.astype(f32)

    normed_e, scale_e, values_e = normalize(early_input, gain_f)
    normed_l, _, values_l = normalize(late_input, gain_f)
    tokens = tokens_everywhere(jnp.concatenate([normed_e, cotangent, normed_l], axis=1))
    whole = weights_everywhere(mine, theirs)
    d, d_rows, h_rows = hidden_units(whole, tokens)
    grads = weight_grads(d, tokens, whole.shape[0], whole.shape[2])
    own_grad, other_grad = rows_summed(grads)

    own, send, gain_part = partial_outputs(d_rows, h_rows, whole, tokens)
    gain_sum_out = gain_sum + summed_everywhere(gain_part.reshape(-1)) / gain_f
    summed = tokens_summed(own, shift(send, C, 1))
    d_normed, mixed = summed[0], summed[1]
    scaled_grad = d_normed * gain_f
    early_grad = (
        cotangent.astype(f32)
        + scale_e * scaled_grad
        - values_e * scale_e**3 * jnp.mean(values_e * scaled_grad, axis=-1, keepdims=True)
    ).astype(bf16)
    late_out = (values_l + 0.5 * mixed).astype(bf16)

    def joined(k):
        a = own_grad[:, k * width : (k + 1) * width]
        b = other_grad[:, k * width : (k + 1) * width]
        return jnp.concatenate([jnp.where(first, a, b), jnp.where(first, b, a)], axis=1)

    return (
        late_out,
        early_grad,
        gate_sum + joined(0),
        up_sum + joined(1),
        down_sum + joined(2),
        gain_sum_out,
    )


def solution(mesh):
    torus = Mesh(mesh.devices.reshape(8, 4, 2, mesh.shape["tp"]), FS_TP)
    in_specs = (
        P(FS_TP, None),
        P(),
        P(FS, Y),
        P(FS, Y),
        P(FS, Y),
        P(FS_TP, None),
        P(FS_TP, None),
        P(FS, Y),
        P(FS, Y),
        P(FS, Y),
        P(),
    )
    out_specs = (P(FS_TP, None), P(FS_TP, None), P(FS, Y), P(FS, Y), P(FS, Y), P())
    return jax.shard_map(
        per_device, mesh=torus, in_specs=in_specs, out_specs=out_specs, check_vma=False
    )
```
